256 devices in a mesh: ep: 64 (over z, y, core), tp: 4 (over x).
Axes of the slice: x: 4, y: 4, z: 8, core: 2. Of those that a mesh axis runs over, the one named last changes fastest.
Arguments:
- outer_gate: bfloat16 [32768, 2048], P('ep', 'tp'), may hold values from -6 to 6
- inner_gate: bfloat16 [32768, 2048], P('ep', 'tp'), may hold values from -6 to 6
- conv_values: bfloat16 [32768, 2048], P('ep', 'tp'), may hold values from -6 to 6
- conv_taps: bfloat16 [3, 2048], P(None, 'tp'), may hold values from -3 to 3
- out_weight: bfloat16 [2048, 2048], P('tp'), may hold values from -0.125 to 0.125
- moe_input: bfloat16 [32768, 2048], P(('ep', 'tp')), may hold values from -6 to 6
- norm_gain: bfloat16 [2048], replicated, may hold values from 0.099609375 to 1.8984375
- gate_proj: bfloat16 [64, 2048, 1024], P('ep', None, 'tp'), may hold values from -0.125 to 0.125
- up_proj: bfloat16 [64, 2048, 1024], P('ep', None, 'tp'), may hold values from -0.125 to 0.125
- down_proj: bfloat16 [64, 1024, 2048], P('ep', 'tp'), may hold values from -0.1875 to 0.1875
- shared_gate: bfloat16 [2048, 1024], P(None, 'tp'), may hold values from -0.125 to 0.125
- shared_up: bfloat16 [2048, 1024], P(None, 'tp'), may hold values from -0.125 to 0.125
- shared_down: bfloat16 [1024, 2048], P('tp'), may hold values from -0.1875 to 0.1875
- routes: int32 [32768, 2], P('ep'), may hold values from 0 to 63, all different within a row; in each aligned block of 128 rows (0 to 127, 128 to 255, ...) at most 8 rows name the same one
- route_weight: float32 [32768, 2], P('ep'), may hold values from 0.3 to 1.5
Outputs:
- mixer_out: bfloat16 [32768, 2048], P(('ep', 'tp'))
- expert_mix: bfloat16 [32768, 2048], P(('ep', 'tp'))
The draws below stay inside these ranges and needn't reach their ends.
Inputs may be any that keep to these rules, and one draw needn't show every extreme that they name: `routes`: each row names 2 different experts. In the 128 rows of one device no expert is named more than 8 times, and in every draw some expert is named exactly 8 times in one device's rows.
All inputs are finite; a program needn't handle non-finite values.
Results may differ from the reference program's by a relative error of at most 0.012.
Values may be sent and summed in bfloat16 or wider, within the bound.
No kernel may reach another device: no remote copies, remote signals or barrier semaphores. Data moves between devices by JAX's collectives and lax.ppermute only.
A program may use at most 128 MiB of HBM per device.

```python
import math
import jax
import jax.numpy as jnp
import numpy as np
from jax import lax

D = 2048
EH = 1024
SH = 1024
TOPK = 2
TAPS = 3
R2 = 128
EXPERTS = 64
CAP = 8
TOK1 = 32768
TOK2 = 32768
N_EP = 64
N_TP = 4


def block_scale(rng, dims, cuts, low, top_value):
    gain = 1.0
    for position, blocks in cuts:
        draws = jax.random.uniform(jax.random.fold_in(jax.random.fold_in(rng, 6), position), (blocks,), jnp.float32, low / len(cuts), top_value / len(cuts))
        gain = gain * jnp.repeat(jnp.exp(draws), dims[position] // blocks).reshape((-1,) + (1,) * (len(dims) - 1 - position))
    return gain


def assign_block(key, own, number, rows, number_of, top, limit, skew):
    ranking = jax.random.permutation(key, number_of)
    heavy_load, common = shares(number_of, rows * top, limit, skew, True), shares(number_of, rows * top, limit, skew, False)
    places = jnp.arange(number_of)

    def named(tallies, turn):
        used = int((tallies > 0).sum())
        fixed = max(1, used // 4)
        passed = fixed + (places - fixed + turn * (used - fixed)) % max(1, number_of - fixed)
        return jnp.zeros((number_of,), jnp.int32).at[ranking[jnp.where(places < fixed, places, passed)]].set(jnp.asarray(tallies, jnp.int32))

    tallies = jnp.where(number % 4 == 0, named(heavy_load, number // 4), named(common, number - number // 4 - 1))
    mixed = jax.random.permutation(jax.random.fold_in(own, 3), number_of)
    donor, receiver = mixed[0:number_of // 2 * 2:2], mixed[1:number_of // 2 * 2:2]
    room = jnp.minimum(tallies[donor] - 1, limit - tallies[receiver]) // 2
    room = jnp.where((donor == ranking[0]) | (receiver == ranking[0]) | (tallies[receiver] == 0), 0, jnp.maximum(room, 0))
    passed = jax.random.randint(jax.random.fold_in(own, 4), (number_of // 2,), 0, 1 << 20) % (room + 1)
    tallies = tallies.at[donor].add(-passed).at[receiver].add(passed)
    items = jnp.searchsorted(jnp.cumsum(tallies), jnp.arange(rows * top), side="right").astype(jnp.int32)
    table = items.reshape(top, rows).T
    table = table[jax.random.permutation(jax.random.fold_in(own, 1), rows)]
    turn = jax.random.randint(jax.random.fold_in(own, 2), (rows, 1), 0, top)
    return jnp.take_along_axis(table, (jnp.arange(top)[None, :] + turn) % top, axis=1)


def shares(count, total, bound, slope, full):
    weights = [(1 << 20) // math.isqrt(standing ** slope) + 1 for standing in range(1, count + 1)]
    largest = bound if full else min(bound, max(-(-total // count), total * weights[0] // sum(weights)))
    least = 1 if total - largest >= count - 1 else 0
    given, surplus = [largest] + [least] * (count - 1), total - largest - least * (count - 1)
    while surplus > 0:
        movable = [i for i in range(1, count) if given[i] < largest] or [i for i in range(1, count) if given[i] < bound]
        pool, budget = sum([weights[i] for i in movable]), surplus
        for i in movable:
            extra = min(bound - given[i], max(1, budget * weights[i] // pool), surplus)
            given[i] = given[i] + extra
            surplus = surplus - extra
    return np.array(given)


def normal_values(key, shape, spread, bound, split=(), held_as=jnp.bfloat16):
    drawn = jax.random.normal(key, shape, jnp.float32) * spread
    if len(split) > 0:
        drawn = block_scale(key, shape, split, -0.22, 0.18) * drawn
    return jnp.clip(drawn, min=-bound, max=bound).astype(held_as)


def setup_inputs(seed: int = 0) -> dict:
    key_of = jax.random.split(jax.random.key(seed), 16)
    outer_gate = normal_values(key_of[0], (TOK1, D), 1.0, 6.0, ((0, 64), (1, 4)))
    inner_gate = normal_values(key_of[1], (TOK1, D), 1.0, 6.0, ((0, 64), (1, 4)))
    conv_values = normal_values(key_of[2], (TOK1, D), 1.0, 6.0, ((0, 64), (1, 4)))
    conv_taps = normal_values(key_of[3], (TAPS, D), 0.577, 3.0, ((1, 4),))
    out_weight = normal_values(key_of[4], (D, D), D ** -0.5, 0.125, ((0, 4),))
    moe_input = normal_values(key_of[5], (TOK2, D), 1.0, 6.0, ((0, 256),))
    norm_gain = jnp.clip(1.0 + 0.18 * jax.random.normal(key_of[6], (D,), jnp.float32), 0.099609375, 1.8984375).astype(jnp.bfloat16)
    gate_proj = normal_values(key_of[7], (EXPERTS, D, EH), D ** -0.5, 0.125, ((0, 64), (2, 4)))
    up_proj = normal_values(key_of[8], (EXPERTS, D, EH), D ** -0.5, 0.125, ((0, 64), (2, 4)))
    down_proj = normal_values(key_of[9], (EXPERTS, EH, D), EH ** -0.5, 0.1875, ((0, 64), (1, 4)))
    shared_gate = normal_values(key_of[10], (D, SH), D ** -0.5, 0.125, ((1, 4),))
    shared_up = normal_values(key_of[11], (D, SH), D ** -0.5, 0.125, ((1, 4),))
    shared_down = normal_values(key_of[12], (SH, D), SH ** -0.5, 0.1875, ((0, 4),))
    routes_keys = jax.random.split(jax.random.fold_in(key_of[13], 1), TOK2 // R2)
    routes_turns = jax.random.permutation(jax.random.fold_in(key_of[13], 3), TOK2 // R2)
    routes = jax.vmap(lambda own, number: assign_block(jax.random.fold_in(key_of[13], 2), own, number, R2, N_EP, TOPK, CAP, 2))(routes_keys, routes_turns).reshape((TOK2, TOPK))
    route_weight = jnp.clip(0.3 + 1.2 * jax.random.uniform(key_of[14], (TOK2, TOPK), jnp.float32) ** block_scale(key_of[14], (TOK2, TOPK), ((0, 64),), -0.2, 0.2), 0.3, 1.5)
    return dict(outer_gate=outer_gate, inner_gate=inner_gate, conv_values=conv_values, conv_taps=conv_taps, out_weight=out_weight, moe_input=moe_input, norm_gain=norm_gain, gate_proj=gate_proj, up_proj=up_proj, down_proj=down_proj, shared_gate=shared_gate, shared_up=shared_up, shared_down=shared_down, routes=routes, route_weight=route_weight)


epsilon = 1e-06

def rms_norm(inputs, scales):
    values = inputs.astype(jnp.float32)
    square = lax.optimization_barrier(jnp.mean(values * values, axis=-1, keepdims=True))
    return (values * lax.rsqrt(square + epsilon) * scales.astype(jnp.float32)).astype(jnp.bfloat16)

def summed_parts(hidden, weight, pieces):
    stride = hidden.shape[1] // pieces
    result = jnp.zeros((hidden.shape[0], weight.shape[1]), jnp.float32)
    for piece_idx in range(pieces):
        partial_sum = jnp.dot(hidden[:, piece_idx * stride:(piece_idx + 1) * stride], weight[piece_idx * stride:(piece_idx + 1) * stride], preferred_element_type=jnp.float32).astype(jnp.bfloat16)
        partial_sum = lax.optimization_barrier(partial_sum)
        result = result + partial_sum.astype(jnp.float32)
    return result

def swiglu(inputs, gate_w, up_w):
    gate_term = jnp.dot(inputs, gate_w, preferred_element_type=jnp.float32)
    upward = jnp.dot(inputs, up_w, preferred_element_type=jnp.float32)
    return (jax.nn.silu(gate_term) * upward).astype(jnp.bfloat16)

def reference(outer_gate, inner_gate, conv_values, conv_taps, out_weight, moe_input, norm_gain, gate_proj, up_proj, down_proj, shared_gate, shared_up, shared_down, routes, route_weight):
    product = inner_gate.astype(jnp.float32) * conv_values.astype(jnp.float32)
    length = product.shape[0]
    padded = jnp.pad(product, ((TAPS - 1, 0), (0, 0)))
    tap_values = conv_taps.astype(jnp.float32)
    convolved = jnp.zeros_like(product)
    for offset in range(TAPS):
        convolved = convolved + tap_values[offset] * padded[offset:offset + length]
    gate_rows = (outer_gate.astype(jnp.float32) * convolved).astype(jnp.bfloat16)
    mixer_out = summed_parts(gate_rows, out_weight, N_TP).astype(jnp.bfloat16)
    normed = rms_norm(moe_input, norm_gain)
    tokens = normed.shape[0]
    slot_limit = N_EP * N_TP * CAP
    token_ids = jnp.arange(tokens, dtype=jnp.int32)

    def one_expert(running, operands):
        expert, gate_w, up_w, down_w = operands
        expert_hits = routes == expert
        chosen = jnp.any(expert_hits, axis=1)
        weight_sum = lax.optimization_barrier(jnp.sum(jnp.where(expert_hits, route_weight, jnp.float32(0.0)), axis=1))
        places = jnp.cumsum(chosen.astype(jnp.int32)) - 1
        targets = jnp.where(chosen, places, slot_limit).astype(jnp.int32)
        row_table = jnp.zeros((slot_limit,), jnp.int32).at[targets].set(token_ids, mode='drop')
        filled = jnp.zeros((slot_limit,), jnp.float32).at[targets].set(1.0, mode='drop')
        hidden = swiglu(normed[row_table], gate_w, up_w)
        result = summed_parts(hidden, down_w, N_TP).astype(jnp.bfloat16)
        result = lax.optimization_barrier(result)
        scaled = result.astype(jnp.float32) * (weight_sum[row_table] * filled)[:, None]
        return (running.at[row_table].add(scaled), None)
    routed, _ = lax.scan(one_expert, jnp.zeros((tokens, normed.shape[1]), jnp.float32), (jnp.arange(N_EP, dtype=jnp.int32), gate_proj, up_proj, down_proj))
    shared_hidden = swiglu(normed, shared_gate, shared_up)
    shared_sum = summed_parts(shared_hidden, shared_down, N_TP)
    expert_mix = (shared_sum + routed).astype(jnp.bfloat16)
    return (mixer_out, expert_mix)
```

```python
import jax
import jax.numpy as jnp
from jax import lax
from jax.experimental import pallas as pl
from jax.experimental.pallas import tpu as pltpu
from jax.sharding import PartitionSpec as P


epsilon = 1e-06


def turn(array, axis, distance):
    size = lax.axis_size(axis)
    return lax.ppermute(array, axis, [(i, (i + distance) % size) for i in range(size)])


def shifted(block, axis, distance):
    devices = range(lax.axis_size(axis))
    route = [(i - distance, i) for i in devices if i - distance in devices]
    return lax.ppermute(block, axis, route)


def exchanged(blocks):
    return lax.all_to_all(blocks, "ep", 0, 0, tiled=True)


def both(first, second):
    return first.astype(jnp.float32) + second.astype(jnp.float32)


def after(value, *others):
    return lax.optimization_barrier((value, *others))[0]


def rms_norm(inputs, scales):
    values = inputs.astype(jnp.float32)
    square = jnp.mean(values * values, axis=-1, keepdims=True)
    return (values * lax.rsqrt(square + epsilon) * scales.astype(jnp.float32)).astype(jnp.bfloat16)


def dot(left, right):
    return jnp.dot(left, right, preferred_element_type=jnp.float32)


def swiglu(inputs, gate_w, up_w):
    return (jax.nn.silu(dot(inputs, gate_w)) * dot(inputs, up_w)).astype(jnp.bfloat16)


def hidden_kernel(*refs):
    count = (len(refs) - 6) // 2
    x_hbm, weights, out = refs[0], refs[1 : 1 + 2 * count], refs[1 + 2 * count]
    x, held, x_sem, sems = refs[2 + 2 * count :]
    copies = [pltpu.make_async_copy(w, held.at[i], sems.at[i]) for i, w in enumerate(weights)]
    first = pltpu.make_async_copy(x_hbm, x, x_sem.at[0])
    first.start()
    for copy in copies:
        copy.start()
    first.wait()
    units = out.shape[1] // count
    for i in range(count):
        copies[2 * i].wait()
        gate_term = dot(x[...], held[2 * i])
        copies[2 * i + 1].wait()
        upward = dot(x[...], held[2 * i + 1])
        out[:, i * units : (i + 1) * units] = (jax.nn.silu(gate_term) * upward).astype(out.dtype)


def hidden_units(rows, pairs):
    weights = [w for pair in pairs for w in pair]
    anywhere = pl.BlockSpec(memory_space=pl.ANY)
    return pl.pallas_call(
        hidden_kernel,
        out_shape=jax.ShapeDtypeStruct((rows.shape[0], len(pairs) * weights[0].shape[1]), rows.dtype),
        in_specs=[anywhere] * (1 + len(weights)),
        out_specs=pl.BlockSpec(memory_space=pltpu.VMEM),
        scratch_shapes=[
            pltpu.VMEM(rows.shape, rows.dtype),
            pltpu.VMEM((len(weights), *weights[0].shape), rows.dtype),
            pltpu.SemaphoreType.DMA((1,)),
            pltpu.SemaphoreType.DMA((len(weights),)),
        ],
        name="hidden_units",
    )(rows, *weights)


def down_kernel(*refs):
    count = len(refs) - 6
    hidden_hbm, blocks, out = refs[0], refs[1 : 1 + count], refs[1 + count]
    hidden, held, sums, sems = refs[2 + count :]
    starts = [0]
    for block in blocks:
        starts.append(starts[-1] + block.shape[0])
    first = pltpu.make_async_copy(hidden_hbm, hidden, sems.at[0])
    first.start()
    copies = []
    for i, block in enumerate(blocks):
        place = held.at[pl.ds(starts[i], block.shape[0])]
        copies.append(pltpu.make_async_copy(block, place, sems.at[1 + i]))
        copies[-1].start()
    first.wait()
    for copy in copies:
        copy.wait()
    tiles, _, width = sums.shape
    stores = []
    for t in range(tiles):
        cols = slice(t * width, (t + 1) * width)
        sums[t] = dot(hidden[...], held[:, cols]).astype(sums.dtype)
        place = out.at[:, pl.ds(t * width, width)]
        stores.append(pltpu.make_async_copy(sums.at[t], place, sems.at[1 + count + t]))
        stores[-1].start()
    for store in stores:
        store.wait()


def down_product(hidden, blocks, tiles=4):
    units = sum(block.shape[0] for block in blocks)
    width = blocks[0].shape[1]
    anywhere = pl.BlockSpec(memory_space=pl.ANY)
    return pl.pallas_call(
        down_kernel,
        out_shape=jax.ShapeDtypeStruct((hidden.shape[0], width), hidden.dtype),
        in_specs=[anywhere] * (1 + len(blocks)),
        out_specs=anywhere,
        scratch_shapes=[
            pltpu.VMEM(hidden.shape, hidden.dtype),
            pltpu.VMEM((units, width), hidden.dtype),
            pltpu.VMEM((tiles, hidden.shape[0], width // tiles), hidden.dtype),
            pltpu.SemaphoreType.DMA((1 + len(blocks) + tiles,)),
        ],
        name="down_product",
    )(hidden, *blocks)


def slots_of(block_routes, experts, capacity):
    tokens = block_routes.shape[0]
    hits = block_routes[:, :, None] == jnp.arange(experts, dtype=jnp.int32)
    hits = hits.astype(jnp.bfloat16)
    rows = lax.broadcasted_iota(jnp.int32, (tokens, tokens), 0)
    cols = lax.broadcasted_iota(jnp.int32, (tokens, tokens), 1)
    earlier = dot((cols < rows).astype(jnp.bfloat16), hits.sum(axis=1))
    rank = jnp.sum(earlier[:, None, :] * hits.astype(jnp.float32), axis=2)
    return block_routes * capacity + rank.astype(jnp.int32)


def per_device(
    outer_gate,
    inner_gate,
    conv_values,
    conv_taps,
    out_weight,
    moe_input,
    norm_gain,
    gate_proj,
    up_proj,
    down_proj,
    shared_gate,
    shared_up,
    shared_down,
    routes,
    route_weight,
):
    tp_count = lax.axis_size("tp")
    ep_count = lax.axis_size("ep")
    my_slot = lax.axis_index("tp")
    group_len = inner_gate.shape[0]
    mix_rows = group_len // tp_count
    model_width = moe_input.shape[1]
    own_rows = moe_input.shape[0]
    top_count = routes.shape[1]
    capacity = 2 * own_rows * top_count // ep_count
    slot_rows = ep_count * capacity
    reach_rows = conv_taps.shape[0] - 1
    half_units = down_proj.shape[1] // 2
    half_rows = own_rows // 2

    gate_o, up_o, down_o = gate_proj[0], up_proj[0], down_proj[0]
    gate_l = turn(gate_o, "tp", 1)
    up_r = turn(up_o, "tp", -1)
    up_l = turn(up_o, "tp", 1)
    gate_r = turn(gate_o, "tp", -1)
    gate_p = turn(gate_l, "tp", 1)
    up_p = turn(up_r, "tp", -1)

    edge_rows = jnp.stack(
        (inner_gate[group_len - reach_rows :], conv_values[group_len - reach_rows :])
    )
    before = shifted(edge_rows, "ep", 1)

    normed = rms_norm(moe_input, norm_gain)
    own_weights = lax.dynamic_slice_in_dim(route_weight, my_slot * own_rows, own_rows, 0)
    own_routes = lax.dynamic_slice_in_dim(routes, my_slot * own_rows, own_rows, 0)
    slots = slots_of(own_routes, ep_count, capacity)
    slot_ids = lax.broadcasted_iota(jnp.int32, (slot_rows, own_rows), 0)
    chosen = (slot_ids == slots[:, 0][None]) | (slot_ids == slots[:, 1][None])
    outgoing = dot(chosen.astype(jnp.bfloat16), normed).astype(jnp.bfloat16)
    landed = exchanged(outgoing.reshape(ep_count, capacity, model_width))
    landed = landed.reshape(slot_rows, model_width)

    down_s = after(down_o, gate_l, up_r)
    down_l = turn(down_s, "tp", 1)
    down_r = turn(down_s, "tp", -1)

    full_gate = jnp.concatenate((before[0], inner_gate), axis=0).astype(jnp.float32)
    full_values = jnp.concatenate((before[1], conv_values), axis=0).astype(jnp.float32)
    product = full_gate * full_values
    tap_values = conv_taps.astype(jnp.float32)
    convolved = tap_values[0] * product[0:group_len]
    for offset in range(1, reach_rows + 1):
        convolved = convolved + tap_values[offset] * product[offset : offset + group_len]
    gate_rows = (outer_gate.astype(jnp.float32) * convolved).astype(jnp.bfloat16)
    mix = []
    for step in range(tp_count):
        place = lax.rem(my_slot + step, tp_count)
        rows = lax.dynamic_slice_in_dim(gate_rows, place * mix_rows, mix_rows, 0)
        mix.append(dot(rows, out_weight).astype(jnp.bfloat16))

    def shared_part(rows):
        return dot(swiglu(rows, shared_gate, shared_up), shared_down).astype(jnp.bfloat16)

    shared_own = shared_part(normed)

    landed = after(landed, shared_own, *mix)
    pairs = ((gate_o, up_o), (gate_l, up_l), (gate_r, up_r), (gate_p, up_p))
    hidden = hidden_units(landed, pairs)
    down_l, down_r = after(down_l, hidden), after(down_r, hidden)
    down_p0 = turn(down_l[:half_units], "tp", 1)
    down_p1 = turn(down_r[half_units:], "tp", -1)
    total = down_product(hidden, (down_o, down_l, down_r, down_p0, down_p1))
    returned = exchanged(total.reshape(ep_count, capacity, model_width))
    returned = returned.reshape(slot_rows, model_width)

    normed_s = after(normed, down_l, down_r)
    normed_l = turn(normed_s, "tp", 1)
    normed_r = turn(normed_s, "tp", -1)

    far, left = after(mix[2], total), after(mix[3], total)
    far = turn(far, "tp", 1)
    from_r = turn(left, "tp", -1)
    normed_l, normed_r = after(normed_l, total), after(normed_r, total)
    normed_p0 = turn(normed_l[:half_rows], "tp", 1)
    normed_p1 = turn(normed_r[half_rows:], "tp", -1)
    normed_p = jnp.concatenate((normed_p0, normed_p1), axis=0)
    from_l = turn(both(mix[1], far).astype(jnp.bfloat16), "tp", 1)
    mixer_out = (both(mix[0], from_l) + from_r.astype(jnp.float32)).astype(jnp.bfloat16)

    share_r, share_l = shared_part(normed_r), shared_part(normed_l)
    far = turn(shared_part(normed_p), "tp", -1)
    from_l = turn(share_r, "tp", 1)
    from_r = turn(both(share_l, far).astype(jnp.bfloat16), "tp", -1)
    shared_total = both(shared_own, from_l) + from_r.astype(jnp.float32)

    slot_ids = lax.broadcasted_iota(jnp.int32, (own_rows, slot_rows), 1)
    routed = shared_total
    for choice in range(top_count):
        picks = (slot_ids == slots[:, choice][:, None]).astype(jnp.bfloat16)
        routed = routed + dot(picks, returned) * own_weights[:, choice][:, None]
    return (mixer_out, routed.astype(jnp.bfloat16))


def solution(mesh):
    return jax.shard_map(
        per_device,
        mesh=mesh,
        in_specs=(
            P("ep", "tp"),
            P("ep", "tp"),
            P("ep", "tp"),
            P(None, "tp"),
            P("tp", None),
            P(("ep", "tp"), None),
            P(),
            P("ep", None, "tp"),
            P("ep", None, "tp"),
            P("ep", "tp", None),
            P(None, "tp"),
            P(None, "tp"),
            P("tp", None),
            P("ep", None),
            P("ep", None),
        ),
        out_specs=(P(("ep", "tp"), None), P(("ep", "tp"), None)),
        check_vma=False,
    )
```

```python
from functools import partial

import jax
import jax.numpy as jnp
from jax import lax
from jax.experimental import pallas as pl
from jax.experimental.pallas import tpu as pltpu
from jax.sharding import PartitionSpec as P


epsilon = 1e-06


def swapped(array, axis, partner):
    return lax.ppermute(
        array, axis, [(i, partner(i)) for i in range(lax.axis_size(axis))]
    )


def shifted(block, axis, distance):
    devices = range(lax.axis_size(axis))
    route = [(i - distance, i) for i in devices if i - distance in devices]
    return lax.ppermute(block, axis, route)


def moved(block, target):
    tp_count, cores = lax.axis_size("tp"), 2
    route = []
    for index in range(lax.axis_size("ep") * tp_count):
        chip, core, place = index // tp_count // cores, index // tp_count % cores, index % tp_count
        goal = target(core, place)
        if goal is not None:
            route.append((index, (chip * cores + goal[0]) * tp_count + goal[1]))
    return lax.ppermute(block, ("ep", "tp"), route)


def across(block):
    return swapped(block, "tp", lambda place: 3 - place)


def beside(block):
    return swapped(block, "tp", lambda place: place ^ 1)


def is_ours(core, place):
    return (core == 0) == (place < 2)


def to_host(core, place):
    return (core, place ^ 1) if is_ours(core, place) else (1 - core, 3 - place)


def to_pair(core, place):
    return None if is_ours(core, place) else (core, place ^ 1)


def to_core(core, place):
    return 1 - core, place


def exchanged(blocks):
    tp_count, cores = lax.axis_size("tp"), 2
    chips = lax.axis_size("ep") // cores
    groups = []
    for core in range(cores):
        for even, odd in ((0, 3), (1, 2)):
            groups.append(
                [
                    (chip * cores + core) * tp_count + place
                    for chip in range(chips)
                    for place in (even, odd)
                ]
            )
    return lax.all_to_all(blocks, ("ep", "tp"), 0, 0, axis_index_groups=groups, tiled=True)


def times(first, second):
    return first.astype(jnp.float32) * second.astype(jnp.float32)


def both(first, second):
    return first.astype(jnp.float32) + second.astype(jnp.float32)


def after(value, *others):
    return lax.optimization_barrier((value, *others))[0]


def dot(left, right):
    return jnp.dot(left, right, preferred_element_type=jnp.float32)


def swiglu(inputs, gate_w, up_w):
    return (jax.nn.silu(dot(inputs, gate_w)) * dot(inputs, up_w)).astype(jnp.bfloat16)


def expert_kernel(*refs, count):
    x_hbm, ups, downs, out = refs[0], refs[1 : 1 + 2 * count], refs[1 + 2 * count : -8], refs[-8]
    x, held, down, hidden, sums, sems, out_sems = refs[-7:]
    units = downs[0].shape[0]
    copies = [pltpu.make_async_copy(x_hbm, x, sems.at[0])]
    for i, block in enumerate(ups):
        copies.append(pltpu.make_async_copy(block, held.at[i], sems.at[1 + i]))
    for i, block in enumerate(downs):
        place = down.at[pl.ds(i * units, units)]
        copies.append(pltpu.make_async_copy(block, place, sems.at[1 + 2 * count + i]))
    for copy in copies:
        copy.start()
    copies[0].wait()
    for i in range(count):
        copies[1 + 2 * i].wait()
        copies[2 + 2 * i].wait()
        gate_term, upward = dot(x[...], held[2 * i]), dot(x[...], held[2 * i + 1])
        hidden[:, i * units : (i + 1) * units] = (jax.nn.silu(gate_term) * upward).astype(x.dtype)
    for i in range(count):
        copies[1 + 2 * count + i].wait()
    tiles, _, width = sums.shape
    stores = []
    for t in range(tiles):
        sums[t] = dot(hidden[...], down[:, t * width : (t + 1) * width]).astype(x.dtype)
        place = out.at[:, pl.ds(t * width, width)]
        stores.append(pltpu.make_async_copy(sums.at[t], place, out_sems.at[t]))
        stores[-1].start()
    for store in stores:
        store.wait()


def expert(rows, ups, downs, tiles=4):
    count, units, width = len(downs), *downs[0].shape
    dtype = rows.dtype
    anywhere = pl.BlockSpec(memory_space=pl.ANY)
    return pl.pallas_call(
        partial(expert_kernel, count=count),
        out_shape=jax.ShapeDtypeStruct(rows.shape, dtype),
        in_specs=[anywhere] * (1 + 3 * count),
        out_specs=anywhere,
        scratch_shapes=[
            pltpu.VMEM(rows.shape, dtype),
            pltpu.VMEM((2 * count, *ups[0].shape), dtype),
            pltpu.VMEM((count * units, width), dtype),
            pltpu.VMEM((rows.shape[0], count * units), dtype),
            pltpu.VMEM((tiles, rows.shape[0], width // tiles), dtype),
            pltpu.SemaphoreType.DMA((1 + 3 * count,)),
            pltpu.SemaphoreType.DMA((tiles,)),
        ],
        name="expert",
    )(rows, *ups, *downs)


def dispatch_kernel(x_ref, gain_ref, routes_ref, normed_ref, out_ref, slots_ref, *, experts):
    tokens = x_ref.shape[0]
    capacity = out_ref.shape[0] // experts
    values = x_ref[...].astype(jnp.float32)
    square = jnp.mean(values * values, axis=-1, keepdims=True)
    scaled = values * lax.rsqrt(square + epsilon) * gain_ref[...].astype(jnp.float32)
    normed = scaled.astype(jnp.bfloat16)
    normed_ref[...] = normed
    mine = pl.ds(pl.multiple_of(lax.axis_index("tp") * tokens, tokens), tokens)
    choices = [routes_ref[k : k + 1, mine] for k in range(routes_ref.shape[0])]
    expert = lax.broadcasted_iota(jnp.int32, (experts, tokens), 0)
    hits = [jnp.where(expert == choice, 1.0, 0.0) for choice in choices]
    rows = lax.broadcasted_iota(jnp.int32, (tokens, tokens), 0)
    cols = lax.broadcasted_iota(jnp.int32, (tokens, tokens), 1)
    before = jnp.where(rows < cols, 1.0, 0.0).astype(jnp.bfloat16)
    earlier = dot((hits[0] + hits[1]).astype(jnp.bfloat16), before)
    slot_ids = lax.broadcasted_iota(jnp.int32, (out_ref.shape[0], tokens), 0)
    chosen = None
    for k, choice in enumerate(choices):
        rank = jnp.sum(earlier * hits[k], axis=0, keepdims=True).astype(jnp.int32)
        slots = choice * capacity + rank
        slots_ref[k : k + 1, :] = slots
        match = slot_ids == slots
        chosen = match if chosen is None else chosen | match
    chosen = jnp.where(chosen, 1.0, 0.0).astype(jnp.bfloat16)
    out_ref[...] = dot(chosen, normed).astype(jnp.bfloat16)


def dispatched(moe_input, norm_gain, routes, experts, capacity):
    tokens, width = moe_input.shape
    in_vmem = pl.BlockSpec(memory_space=pltpu.VMEM)
    return pl.pallas_call(
        partial(dispatch_kernel, experts=experts),
        out_shape=(
            jax.ShapeDtypeStruct((tokens, width), jnp.bfloat16),
            jax.ShapeDtypeStruct((experts * capacity, width), jnp.bfloat16),
            jax.ShapeDtypeStruct((routes.shape[1], tokens), jnp.int32),
        ),
        in_specs=[in_vmem] * 3,
        out_specs=[in_vmem] * 3,
        name="dispatched",
    )(moe_input, norm_gain.reshape(1, width), routes.T)


def per_device(
    outer_gate,
    inner_gate,
    conv_values,
    conv_taps,
    out_weight,
    moe_input,
    norm_gain,
    gate_proj,
    up_proj,
    down_proj,
    shared_gate,
    shared_up,
    shared_down,
    routes,
    route_weight,
):
    tp_count = lax.axis_size("tp")
    ep_count = lax.axis_size("ep")
    my_slot = lax.axis_index("tp")
    group_len = inner_gate.shape[0]
    mix_rows = group_len // tp_count
    model_width = moe_input.shape[1]
    own_rows = moe_input.shape[0]
    top_count = routes.shape[1]
    capacity = 2 * own_rows * top_count // ep_count
    slot_rows = ep_count * capacity
    reach_rows = conv_taps.shape[0] - 1

    ours = (lax.axis_index("ep") % 2 == 0) == (my_slot < 2)
    weights = {"gate": gate_proj[0], "up": up_proj[0], "down": down_proj[0]}
    first = {name: moved(block, to_host) for name, block in weights.items()}
    second, third, fourth = {}, {}, {}

    def bring(name):
        second[name] = moved(first[name], to_pair)

    def spread(name, *earlier):
        third[name] = moved(first[name], to_core)
        second[name] = jnp.where(ours, weights[name], after(second[name], *earlier))
        fourth[name] = moved(second[name], to_core)

    tail = slice(group_len - reach_rows, group_len)
    before = shifted(times(inner_gate[tail], conv_values[tail]), "ep", 1)

    normed, outgoing, slots = dispatched(moe_input, norm_gain, routes, ep_count, capacity)
    slots = slots.T
    own_weights = lax.dynamic_slice_in_dim(route_weight, my_slot * own_rows, own_rows, 0)
    landed = exchanged(outgoing.reshape(ep_count, capacity, model_width))
    landed = landed.reshape(slot_rows, model_width)

    for name in weights:
        bring(name)
    product = jnp.concatenate((before, times(inner_gate, conv_values)), axis=0)
    tap_values = conv_taps.astype(jnp.float32)
    convolved = tap_values[0] * product[0:group_len]
    for offset in range(1, reach_rows + 1):
        convolved = convolved + tap_values[offset] * product[offset : offset + group_len]
    gate_rows = (outer_gate.astype(jnp.float32) * convolved).astype(jnp.bfloat16)
    mix = {}
    places = {"own": my_slot, "across": 3 - my_slot, "beside": my_slot ^ 1, "far": 3 - my_slot ^ 1}
    for key, place in places.items():
        rows = lax.dynamic_slice_in_dim(gate_rows, place * mix_rows, mix_rows, 0)
        mix[key] = dot(rows, out_weight).astype(jnp.bfloat16)

    def shared_part(rows):
        return dot(swiglu(rows, shared_gate, shared_up), shared_down).astype(jnp.bfloat16)

    normed_across = across(normed)
    normed_beside = beside(normed)
    shared = {"own": shared_part(normed)}
    early = (*mix.values(), *shared.values())
    spread("gate", *early)
    spread("up", second["gate"])
    spread("down", second["up"])

    landed = after(landed, *early)
    blocks = (first, third, second, fourth)
    ups = [w[name] for w in blocks for name in ("gate", "up")]
    total = expert(landed, ups, [w["down"] for w in blocks])
    returned = exchanged(total.reshape(ep_count, capacity, model_width))
    returned = returned.reshape(slot_rows, model_width)

    normed_far = beside(normed_across)

    got_own = across(mix["across"])
    got_beside = after(across(mix["far"]), total)
    got_rest = beside(both(mix["beside"], got_beside).astype(jnp.bfloat16))
    mixer_out = both(mix["own"], got_own) + got_rest.astype(jnp.float32)

    shared["far"] = shared_part(after(normed_far, total))
    shared["beside"] = shared_part(after(normed_beside, total))
    shared["across"] = shared_part(after(normed_across, total))
    got_across = beside(shared["far"])
    got_own = beside(shared["beside"])
    got_rest = across(both(shared["across"], got_across).astype(jnp.bfloat16))
    shared_total = both(shared["own"], got_own) + got_rest.astype(jnp.float32)

    slot_ids = lax.broadcasted_iota(jnp.int32, (own_rows, slot_rows), 1)
    routed = shared_total
    for choice in range(top_count):
        picks = (slot_ids == slots[:, choice][:, None]).astype(jnp.bfloat16)
        routed = routed + dot(picks, returned) * own_weights[:, choice][:, None]
    return (mixer_out.astype(jnp.bfloat16), routed.astype(jnp.bfloat16))


def solution(mesh):
    return jax.shard_map(
        per_device,
        mesh=mesh,
        in_specs=(
            P("ep", "tp"),
            P("ep", "tp"),
            P("ep", "tp"),
            P(None, "tp"),
            P("tp", None),
            P(("ep", "tp"), None),
            P(),
            P("ep", None, "tp"),
            P("ep", None, "tp"),
            P("ep", "tp", None),
            P(None, "tp"),
            P(None, "tp"),
            P("tp", None),
            P("ep", None),
            P("ep", None),
        ),
        out_specs=(P(("ep", "tp"), None), P(("ep", "tp"), None)),
        check_vma=False,
    )
```

```python
from functools import partial

import jax
import jax.numpy as jnp
from jax import lax
from jax.experimental import pallas as pl
from jax.experimental.pallas import tpu as pltpu
from jax.sharding import PartitionSpec as P


epsilon = 1e-06


def swapped(array, axis, partner):
    return lax.ppermute(
        array, axis, [(i, partner(i)) for i in range(lax.axis_size(axis))]
    )


def shifted(block, axis, distance):
    devices = range(lax.axis_size(axis))
    route = [(i - distance, i) for i in devices if i - distance in devices]
    return lax.ppermute(block, axis, route)


def moved(block, target):
    tp_count, cores = lax.axis_size("tp"), 2
    route = []
    for index in range(lax.axis_size("ep") * tp_count):
        chip, core, place = index // tp_count // cores, index // tp_count % cores, index % tp_count
        goal = target(core, place)
        if goal is not None:
            route.append((index, (chip * cores + goal[0]) * tp_count + goal[1]))
    return lax.ppermute(block, ("ep", "tp"), route)


def across(block):
    return swapped(block, "tp", lambda place: 3 - place)


def beside(block):
    return swapped(block, "tp", lambda place: place ^ 1)


def is_ours(core, place):
    return (core == 0) == (place < 2)


def to_host(core, place):
    return (core, place ^ 1) if is_ours(core, place) else (1 - core, 3 - place)


def to_pair(core, place):
    return None if is_ours(core, place) else (core, place ^ 1)


def to_core(core, place):
    return 1 - core, place


def exchanged(blocks):
    tp_count, cores = lax.axis_size("tp"), 2
    chips = lax.axis_size("ep") // cores
    groups = []
    for core in range(cores):
        for even, odd in ((0, 3), (1, 2)):
            groups.append(
                [
                    (chip * cores + core) * tp_count + place
                    for chip in range(chips)
                    for place in (even, odd)
                ]
            )
    return lax.all_to_all(blocks, ("ep", "tp"), 0, 0, axis_index_groups=groups, tiled=True)


def times(first, second):
    return first.astype(jnp.float32) * second.astype(jnp.float32)


def both(first, second):
    return first.astype(jnp.float32) + second.astype(jnp.float32)


def after(value, *others):
    return lax.optimization_barrier((value, *others))[0]


def dot(left, right):
    return jnp.dot(left, right, preferred_element_type=jnp.float32)


def swiglu(inputs, gate_w, up_w):
    return (jax.nn.silu(dot(inputs, gate_w)) * dot(inputs, up_w)).astype(jnp.bfloat16)


def expert_kernel(*refs, count):
    x_hbm, ups, downs, out = refs[0], refs[1 : 1 + 2 * count], refs[1 + 2 * count : -8], refs[-8]
    x, held, down, hidden, sums, sems, out_sems = refs[-7:]
    units = downs[0].shape[0]
    copies = [pltpu.make_async_copy(x_hbm, x, sems.at[0])]
    for i, block in enumerate(ups):
        copies.append(pltpu.make_async_copy(block, held.at[i], sems.at[1 + i]))
    for i, block in enumerate(downs):
        place = down.at[pl.ds(i * units, units)]
        copies.append(pltpu.make_async_copy(block, place, sems.at[1 + 2 * count + i]))
    for copy in copies:
        copy.start()
    copies[0].wait()
    for i in range(count):
        copies[1 + 2 * i].wait()
        copies[2 + 2 * i].wait()
        gate_term, upward = dot(x[...], held[2 * i]), dot(x[...], held[2 * i + 1])
        hidden[:, i * units : (i + 1) * units] = (jax.nn.silu(gate_term) * upward).astype(x.dtype)
    for i in range(count):
        copies[1 + 2 * count + i].wait()
    tiles, _, width = sums.shape
    stores = []
    for t in range(tiles):
        sums[t] = dot(hidden[...], down[:, t * width : (t + 1) * width]).astype(x.dtype)
        place = out.at[:, pl.ds(t * width, width)]
        stores.append(pltpu.make_async_copy(sums.at[t], place, out_sems.at[t]))
        stores[-1].start()
    for store in stores:
        store.wait()


def expert(rows, ups, downs, tiles=4):
    count, units, width = len(downs), *downs[0].shape
    dtype = rows.dtype
    anywhere = pl.BlockSpec(memory_space=pl.ANY)
    return pl.pallas_call(
        partial(expert_kernel, count=count),
        out_shape=jax.ShapeDtypeStruct(rows.shape, dtype),
        in_specs=[anywhere] * (1 + 3 * count),
        out_specs=anywhere,
        scratch_shapes=[
            pltpu.VMEM(rows.shape, dtype),
            pltpu.VMEM((2 * count, *ups[0].shape), dtype),
            pltpu.VMEM((count * units, width), dtype),
            pltpu.VMEM((rows.shape[0], count * units), dtype),
            pltpu.VMEM((tiles, rows.shape[0], width // tiles), dtype),
            pltpu.SemaphoreType.DMA((1 + 3 * count,)),
            pltpu.SemaphoreType.DMA((tiles,)),
        ],
        name="expert",
    )(rows, *ups, *downs)


def dispatch_kernel(x_ref, gain_ref, routes_ref, normed_ref, out_ref, slots_ref, *, experts):
    tokens = x_ref.shape[0]
    capacity = out_ref.shape[0] // experts
    values = x_ref[...].astype(jnp.float32)
    square = jnp.mean(values * values, axis=-1, keepdims=True)
    scaled = values * lax.rsqrt(square + epsilon) * gain_ref[...].astype(jnp.float32)
    normed = scaled.astype(jnp.bfloat16)
    normed_ref[...] = normed
    mine = pl.ds(pl.multiple_of(lax.axis_index("tp") * tokens, tokens), tokens)
    choices = [routes_ref[k : k + 1, mine] for k in range(routes_ref.shape[0])]
    expert = lax.broadcasted_iota(jnp.int32, (experts, tokens), 0)
    hits = [jnp.where(expert == choice, 1.0, 0.0) for choice in choices]
    rows = lax.broadcasted_iota(jnp.int32, (tokens, tokens), 0)
    cols = lax.broadcasted_iota(jnp.int32, (tokens, tokens), 1)
    before = jnp.where(rows < cols, 1.0, 0.0).astype(jnp.bfloat16)
    earlier = dot((hits[0] + hits[1]).astype(jnp.bfloat16), before)
    slot_ids = lax.broadcasted_iota(jnp.int32, (out_ref.shape[0], tokens), 0)
    chosen = None
    for k, choice in enumerate(choices):
        rank = jnp.sum(earlier * hits[k], axis=0, keepdims=True).astype(jnp.int32)
        slots = choice * capacity + rank
        slots_ref[k : k + 1, :] = slots
        match = slot_ids == slots
        chosen = match if chosen is None else chosen | match
    chosen = jnp.where(chosen, 1.0, 0.0).astype(jnp.bfloat16)
    out_ref[...] = dot(chosen, normed).astype(jnp.bfloat16)


def dispatched(moe_input, norm_gain, routes, experts, capacity):
    tokens, width = moe_input.shape
    in_vmem = pl.BlockSpec(memory_space=pltpu.VMEM)
    return pl.pallas_call(
        partial(dispatch_kernel, experts=experts),
        out_shape=(
            jax.ShapeDtypeStruct((tokens, width), jnp.bfloat16),
            jax.ShapeDtypeStruct((experts * capacity, width), jnp.bfloat16),
            jax.ShapeDtypeStruct((routes.shape[1], tokens), jnp.int32),
        ),
        in_specs=[in_vmem] * 3,
        out_specs=[in_vmem] * 3,
        name="dispatched",
    )(moe_input, norm_gain.reshape(1, width), routes.T)


def combine_kernel(slots_ref, weights_ref, rows_ref, *refs):
    parts, out_ref = refs[:-1], refs[-1]
    total = sum(part[...].astype(jnp.float32) for part in parts)
    slot_ids = lax.broadcasted_iota(jnp.int32, (out_ref.shape[0], rows_ref.shape[0]), 1)
    for k in range(slots_ref.shape[1]):
        picks = jnp.where(slot_ids == slots_ref[:, k : k + 1], 1.0, 0.0).astype(rows_ref.dtype)
        total = total + dot(picks, rows_ref[...]) * weights_ref[:, k : k + 1]
    out_ref[...] = total.astype(out_ref.dtype)


def combined(rows, slots, weights, parts, tiles=4):
    count, width = rows.shape
    tokens, top = slots.shape
    small = pl.BlockSpec((tokens, top), lambda j: (0, 0))
    tile = pl.BlockSpec((tokens, width // tiles), lambda j: (0, j))
    return pl.pallas_call(
        combine_kernel,
        grid=(tiles,),
        out_shape=jax.ShapeDtypeStruct((tokens, width), jnp.bfloat16),
        in_specs=[small, small, pl.BlockSpec((count, width // tiles), lambda j: (0, j))]
        + [tile] * len(parts),
        out_specs=tile,
        name="combined",
    )(slots, weights, rows, *parts)


def per_device(
    outer_gate,
    inner_gate,
    conv_values,
    conv_taps,
    out_weight,
    moe_input,
    norm_gain,
    gate_proj,
    up_proj,
    down_proj,
    shared_gate,
    shared_up,
    shared_down,
    routes,
    route_weight,
):
    tp_count = lax.axis_size("tp")
    ep_count = lax.axis_size("ep")
    my_slot = lax.axis_index("tp")
    group_len = inner_gate.shape[0]
    mix_rows = group_len // tp_count
    model_width = moe_input.shape[1]
    own_rows = moe_input.shape[0]
    top_count = routes.shape[1]
    capacity = 2 * own_rows * top_count // ep_count
    slot_rows = ep_count * capacity
    reach_rows = conv_taps.shape[0] - 1

    ours = (lax.axis_index("ep") % 2 == 0) == (my_slot < 2)
    weights = {"gate": gate_proj[0], "up": up_proj[0], "down": down_proj[0]}
    first = {name: moved(block, to_host) for name, block in weights.items()}
    second, third, fourth = {}, {}, {}

    def bring(name):
        second[name] = moved(first[name], to_pair)

    def spread(name, *earlier):
        third[name] = moved(first[name], to_core)
        second[name] = jnp.where(ours, weights[name], after(second[name], *earlier))
        fourth[name] = moved(second[name], to_core)

    tail = slice(group_len - reach_rows, group_len)
    before = shifted(times(inner_gate[tail], conv_values[tail]), "ep", 1)

    normed, outgoing, slots = dispatched(moe_input, norm_gain, routes, ep_count, capacity)
    slots = slots.T
    own_weights = lax.dynamic_slice_in_dim(route_weight, my_slot * own_rows, own_rows, 0)
    landed = exchanged(outgoing.reshape(ep_count, capacity, model_width))
    landed = landed.reshape(slot_rows, model_width)

    for name in weights:
        bring(name)
    product = jnp.concatenate((before, times(inner_gate, conv_values)), axis=0)
    tap_values = conv_taps.astype(jnp.float32)
    convolved = tap_values[0] * product[0:group_len]
    for offset in range(1, reach_rows + 1):
        convolved = convolved + tap_values[offset] * product[offset : offset + group_len]
    gate_rows = (outer_gate.astype(jnp.float32) * convolved).astype(jnp.bfloat16)
    mix = {}
    places = {"own": my_slot, "across": 3 - my_slot, "beside": my_slot ^ 1, "far": 3 - my_slot ^ 1}
    for key, place in places.items():
        rows = lax.dynamic_slice_in_dim(gate_rows, place * mix_rows, mix_rows, 0)
        mix[key] = dot(rows, out_weight).astype(jnp.bfloat16)

    def shared_part(rows):
        return dot(swiglu(rows, shared_gate, shared_up), shared_down).astype(jnp.bfloat16)

    shared = {"own": shared_part(normed)}
    early = (*mix.values(), *shared.values())
    spread("gate", *early)
    spread("up", second["gate"])
    spread("down", fourth["up"])

    landed = after(landed, *early)
    blocks = (first, third, second, fourth)
    ups = [w[name] for w in blocks for name in ("gate", "up")]
    total = expert(landed, ups, [w["down"] for w in blocks])
    returned = exchanged(total.reshape(ep_count, capacity, model_width))
    returned = returned.reshape(slot_rows, model_width)

    normed_across = across(normed)
    normed_beside = beside(normed)
    normed_far = beside(normed_across)

    got_own = across(mix["across"])
    got_beside = after(across(mix["far"]), total)
    mix_sum = both(mix["beside"], got_beside).astype(jnp.bfloat16)
    got_rest = beside(mix_sum)
    mixer_out = both(mix["own"], got_own) + got_rest.astype(jnp.float32)

    shared["far"] = shared_part(after(normed_far, mix_sum))
    shared["across"] = shared_part(after(normed_across, shared["far"]))
    shared["beside"] = shared_part(after(normed_beside, shared["far"]))
    got_own = beside(shared["beside"])
    got_across = beside(shared["far"])
    passed_on = both(shared["across"], got_across).astype(jnp.bfloat16)
    shared_parts = (shared["own"], got_own, across(passed_on))

    expert_mix = combined(returned, slots, own_weights, shared_parts)
    return (mixer_out.astype(jnp.bfloat16), expert_mix)


def solution(mesh):
    return jax.shard_map(
        per_device,
        mesh=mesh,
        in_specs=(
            P("ep", "tp"),
            P("ep", "tp"),
            P("ep", "tp"),
            P(None, "tp"),
            P("tp", None),
            P(("ep", "tp"), None),
            P(),
            P("ep", None, "tp"),
            P("ep", None, "tp"),
            P("ep", "tp", None),
            P(None, "tp"),
            P(None, "tp"),
            P("tp", None),
            P("ep", None),
            P("ep", None),
        ),
        out_specs=(P(("ep", "tp"), None), P(("ep", "tp"), None)),
        check_vma=False,
    )
```
